512 devices in a mesh: grp: 2 (over y), dp: 8 (over x), kv: 16 (over z), tp: 2 (over core).
Axes of the slice: x: 8, y: 2, z: 16, core: 2. Of those that a mesh axis runs over, the one named last changes fastest.
The devices are a block of a 8x8x16 slice.
Arguments:
- tokens: bfloat16 [192, 2048], P(('grp', 'dp'), 'kv'), parts along dimension 0, may hold values from -24 to 24
- norm_gain: bfloat16 [2048], P('kv'), may hold values from 0.099609375 to 1.8984375
- query_weight: bfloat16 [2048, 2048], P('kv', 'tp'), may hold values from -0.125 to 0.125
- key_weight: bfloat16 [2048, 128], replicated, may hold values from -0.125 to 0.125
- value_weight: bfloat16 [2048, 128], replicated, may hold values from -0.125 to 0.125
- gate_weight: bfloat16 [2048, 2], replicated, may hold values from -0.5 to 0.5
- output_weight: bfloat16 [2048, 2048], P('tp', 'kv'), may hold values from -1 to 1
- query_gain: bfloat16 [64], replicated, may hold values from 0.099609375 to 1.8984375
- key_gain: bfloat16 [64], replicated, may hold values from 0.099609375 to 1.8984375
- key_cache: bfloat16 [192, 2, 64, 16384], P(('grp', 'dp'), 'tp', None, 'kv'), parts along dimension 0, may hold values from -1220 to 1220
- value_cache: bfloat16 [192, 2, 64, 16384], P(('grp', 'dp'), 'tp', None, 'kv'), parts along dimension 0, may hold values from -6 to 6
- decay_cache: float32 [192, 2, 16384], P(('grp', 'dp'), 'tp', 'kv'), parts along dimension 0, may hold values from -2340 to 0, as said below
- lengths: int32 [192], P(('grp', 'dp')), parts along dimension 0, may hold values from 8192 to 16384, as said below
Outputs:
- mixed: bfloat16 [192, 2048], P(('grp', 'dp'), 'kv'), parts along dimension 0
- new_key: bfloat16 [192, 2, 64], P(('grp', 'dp'), 'tp'), parts along dimension 0
- new_value: bfloat16 [192, 2, 64], P(('grp', 'dp'), 'tp'), parts along dimension 0
- new_gate: float32 [192, 2], P(('grp', 'dp'), 'tp'), parts along dimension 0
The draws below stay inside these ranges and needn't reach their ends.
There are 2 independent parts, one for each index of `grp`. The reference program is written for one: setup_inputs(seed, part) draws one part's arguments, and reference() takes and returns one part's arrays. A program takes and returns all parts, laid end to end along the dimension named above; an argument that names none is the same for every part. Nothing has to cross between parts.
Inputs may be any that keep to these rules, and one draw needn't show every extreme that they name: `decay_cache`: never positive, not falling as the position grows within a sequence, and zero at positions lengths - 1 and beyond. `lengths`: A sequence's cache holds positions 0 to its length - 1.
All inputs are finite; a program needn't handle non-finite values.
Results may differ from the reference program's by a relative error of at most 0.015.
The reference program's roundings to bfloat16 on the way count: a program that leaves them out, or rounds other values in their place, can miss the bound.
Values may be sent and summed in bfloat16 or wider, within the bound.
No kernel may reach another device: no remote copies, remote signals or barrier semaphores. Data moves between devices by JAX's collectives and lax.ppermute only.
A program may use at most 64 MiB of HBM per device.

```python
import math
import jax
import jax.numpy as jnp
from jax import lax

D = 2048
HQ = 32
HD = 64
KEY_VALUE_HEADS = 2
POS_DEV = 1024
BATCH_ROWS = 96
CACHE_LENGTH = 16384
N_TP = 2


def sequence_lengths(key):
    return jax.random.randint(jax.random.fold_in(key, 7), (BATCH_ROWS,), CACHE_LENGTH // 2, CACHE_LENGTH + 1).astype(jnp.int32)


def draw_lengths(key, part):
    return sequence_lengths(key)


def draw_tokens(key, part):
    key_entries = jax.random.split(jax.random.fold_in(key, 3), 2)
    base = jnp.clip(jax.random.normal(key_entries[0], (BATCH_ROWS, D), jnp.float32), -5.0, 5.0)
    columns = jnp.arange(D, dtype=jnp.float32) / (D - 1)
    rough = jnp.exp(jax.random.uniform(key_entries[1], (D,), jnp.float32, math.log(0.6), math.log(1.6)))
    column_scale = jnp.exp(math.log(0.5) + math.log(3.0) * columns) * rough
    return (base * column_scale[None, :]).astype(jnp.bfloat16)


def draw_key_cache(key, part):
    key_entries = jax.random.split(jax.random.fold_in(key, 23), 1)
    base = jnp.clip(jax.random.normal(key_entries[0], (BATCH_ROWS, KEY_VALUE_HEADS, HD, CACHE_LENGTH), jnp.float32), -4.0, 4.0)
    return base.astype(jnp.bfloat16)


def draw_decay_cache(key, part):
    seq_len = sequence_lengths(key)
    key_entries = jax.random.split(jax.random.fold_in(key, 11), 7)
    fast_share = 0.5
    quick_decay = jax.random.uniform(key_entries[0], (BATCH_ROWS, KEY_VALUE_HEADS), jnp.float32) < fast_share
    fast_rate = jnp.exp(jax.random.uniform(key_entries[1], (BATCH_ROWS, KEY_VALUE_HEADS), jnp.float32, math.log(1.0 / 100.0), math.log(1.0 / 30.0)))
    slow_total = jax.random.uniform(key_entries[2], (BATCH_ROWS, KEY_VALUE_HEADS), jnp.float32, 0.4, 1.0)
    rate = jnp.where(quick_decay, fast_rate, slow_total / CACHE_LENGTH)
    block_rate = jnp.exp(jax.random.uniform(key_entries[3], (BATCH_ROWS, KEY_VALUE_HEADS, CACHE_LENGTH // POS_DEV), jnp.float32, math.log(0.5), math.log(2.0)))
    block_rate = jnp.repeat(block_rate, POS_DEV, axis=2)
    rough = jax.random.uniform(key_entries[4], (BATCH_ROWS, KEY_VALUE_HEADS, CACHE_LENGTH), jnp.float32, 0.0, 2.0)
    gate_logarithms = -rate[:, :, None] * block_rate * rough
    spike_position = jax.random.randint(key_entries[5], (BATCH_ROWS, KEY_VALUE_HEADS, 2), 0, CACHE_LENGTH)
    spike_strength = jax.random.uniform(key_entries[6], (BATCH_ROWS, KEY_VALUE_HEADS, 2), jnp.float32, math.log(0.55), math.log(0.8))
    cache_positions = jnp.arange(CACHE_LENGTH, dtype=jnp.int32)
    match_count = (cache_positions[None, None, None, :] == spike_position[:, :, :, None]).astype(jnp.float32)
    spike_events = jnp.sum(spike_strength[:, :, :, None] * match_count, axis=2)
    gate_logarithms = gate_logarithms + jnp.where(quick_decay[:, :, None], 0.0, spike_events)
    valid = cache_positions[None, None, :] < seq_len[:, None, None]
    running = jnp.cumsum(jnp.where(valid, gate_logarithms, 0.0), axis=2)
    return running[:, :, -1:] - running


def block_scale(stream_key, dims, cuts, smallest, top_value):
    factor_of = 1.0
    for position, parts in cuts:
        draws = jax.random.uniform(jax.random.fold_in(jax.random.fold_in(stream_key, 6), position), (parts,), jnp.float32, smallest / len(cuts), top_value / len(cuts))
        factor_of = factor_of * jnp.repeat(jnp.exp(draws), dims[position] // parts).reshape((-1,) + (1,) * (len(dims) - 1 - position))
    return factor_of


def normal_values(key, dims, scale, bound, pieces=(), held_as=jnp.bfloat16):
    entries = scale * jax.random.normal(key, dims, jnp.float32)
    if pieces:
        entries = entries * block_scale(key, dims, pieces, -0.22, 0.18)
    return jnp.clip(entries, -bound, bound).astype(held_as)


def setup_inputs(seed: int = 0, part: int = 0) -> dict:
    arg_keys = jax.random.split(jax.random.key(seed), 14)
    part_splits = jax.random.split(jax.random.fold_in(arg_keys[13], part), 14)
    tokens = draw_tokens(jax.random.fold_in(jax.random.fold_in(arg_keys[13], part), 71), part)
    norm_gain = jnp.clip(1.0 + 0.18 * jax.random.normal(arg_keys[1], (D,), jnp.float32), 0.099609375, 1.8984375).astype(jnp.bfloat16)
    query_weight = normal_values(arg_keys[2], (D, HQ * HD), D ** -0.5, 0.125, ((0, 16), (1, 2)))
    key_weight = normal_values(arg_keys[3], (D, KEY_VALUE_HEADS * HD), D ** -0.5, 0.125)
    value_weight = normal_values(arg_keys[4], (D, KEY_VALUE_HEADS * HD), D ** -0.5, 0.125)
    gate_weight = normal_values(arg_keys[5], (D, KEY_VALUE_HEADS), (D // 16) ** -0.5, 0.5)
    output_weight = normal_values(arg_keys[6], (HQ * HD, D), (HQ * HD // 64) ** -0.5, 1.0, ((0, 2), (1, 16)))
    query_gain = jnp.clip(1.0 + 0.18 * jax.random.normal(arg_keys[7], (HD,), jnp.float32), 0.099609375, 1.8984375).astype(jnp.bfloat16)
    key_gain = jnp.clip(1.0 + 0.18 * jax.random.normal(arg_keys[8], (HD,), jnp.float32), 0.099609375, 1.8984375).astype(jnp.bfloat16)
    key_cache = draw_key_cache(jax.random.fold_in(jax.random.fold_in(arg_keys[13], part), 71), part)
    value_cache = normal_values(part_splits[10], (BATCH_ROWS, KEY_VALUE_HEADS, HD, CACHE_LENGTH), 1.0, 6.0, ((0, 8), (1, 2), (3, 16)))
    decay_cache = draw_decay_cache(jax.random.fold_in(jax.random.fold_in(arg_keys[13], part), 71), part)
    lengths = draw_lengths(jax.random.fold_in(jax.random.fold_in(arg_keys[13], part), 71), part)
    return dict(tokens=tokens, norm_gain=norm_gain, query_weight=query_weight, key_weight=key_weight, value_weight=value_weight, gate_weight=gate_weight, output_weight=output_weight, query_gain=query_gain, key_gain=key_gain, key_cache=key_cache, value_cache=value_cache, decay_cache=decay_cache, lengths=lengths)


EPSILON = 1e-06
FLOOR = -1e+30

def head_norm(values, head_gain):
    values = values.astype(jnp.float32)
    factor = lax.rsqrt(lax.optimization_barrier(jnp.mean(values * values, axis=-1, keepdims=True)) + EPSILON)
    return (values * factor * head_gain.astype(jnp.float32)).astype(jnp.bfloat16)

def attend_one(items):
    grouped, key_entries, values, decays, length, gate, own_key, own_value = items
    group_size = HQ // KEY_VALUE_HEADS
    block_count = CACHE_LENGTH // POS_DEV
    scores = jnp.einsum('kge,kep->kgp', grouped.astype(jnp.float32), key_entries.astype(jnp.float32)) * HD ** (-0.5)
    scores = scores + decays[:, None, :] + gate[:, None, None]
    scores = scores.reshape(KEY_VALUE_HEADS, group_size, block_count, POS_DEV)
    cache_positions = jnp.arange(CACHE_LENGTH, dtype=jnp.int32).reshape(block_count, POS_DEV)
    valid = (cache_positions < length)[None, None]
    masked = jnp.where(valid, scores, FLOOR)
    block_max = lax.optimization_barrier(jnp.max(masked, axis=3))
    weights = jnp.where(valid, jnp.exp(scores - block_max[..., None]), 0.0)
    block_total = lax.optimization_barrier(jnp.sum(weights, axis=3))
    weights_low = lax.optimization_barrier(weights.astype(jnp.bfloat16)).astype(jnp.float32)
    value_blocks = values.astype(jnp.float32).reshape(KEY_VALUE_HEADS, HD, block_count, POS_DEV)
    block_values = jnp.einsum('kgjp,kejp->kgje', weights_low, value_blocks)
    own = jnp.einsum('kge,ke->kg', grouped.astype(jnp.float32), own_key.astype(jnp.float32)) * HD ** (-0.5)
    highest = jnp.maximum(lax.optimization_barrier(jnp.max(block_max, axis=2)), own)
    far_scale = jnp.exp(block_max - highest[..., None])
    own_scale = jnp.exp(own - highest)
    total = lax.optimization_barrier(jnp.sum(block_total * far_scale, axis=2)) + own_scale
    summed = lax.optimization_barrier(jnp.sum(block_values * far_scale[..., None], axis=2))
    summed = summed + own_scale[..., None] * own_value.astype(jnp.float32)[:, None, :]
    attended = (summed / total[..., None]).astype(jnp.bfloat16)
    return attended.reshape(HQ * HD)

def reference(tokens, norm_gain, query_weight, key_weight, value_weight, gate_weight, output_weight, query_gain, key_gain, key_cache, value_cache, decay_cache, lengths):
    tokens_wide = tokens.astype(jnp.float32)
    scaled = (tokens_wide * norm_gain.astype(jnp.float32)).astype(jnp.bfloat16)
    row_scale = lax.rsqrt(lax.optimization_barrier(jnp.mean(tokens_wide * tokens_wide, axis=1)) + EPSILON)
    query_raw = jnp.dot(scaled, query_weight, preferred_element_type=jnp.float32).reshape(BATCH_ROWS, HQ, HD)
    key_raw = jnp.dot(scaled, key_weight, preferred_element_type=jnp.float32).reshape(BATCH_ROWS, KEY_VALUE_HEADS, HD)
    value_raw = jnp.dot(scaled, value_weight, preferred_element_type=jnp.float32)
    gate_raw = jnp.dot(scaled, gate_weight, preferred_element_type=jnp.float32)
    queries = head_norm(query_raw, query_gain)
    new_key = head_norm(key_raw, key_gain)
    new_value = (row_scale[:, None] * value_raw).astype(jnp.bfloat16).reshape(BATCH_ROWS, KEY_VALUE_HEADS, HD)
    new_gate = jax.nn.log_sigmoid(row_scale[:, None] * gate_raw)
    grouped = queries.reshape(BATCH_ROWS, KEY_VALUE_HEADS, HQ // KEY_VALUE_HEADS, HD)
    attended = lax.map(attend_one, (grouped, key_cache, value_cache, decay_cache, lengths, new_gate, new_key, new_value))
    attended_groups = attended.reshape(BATCH_ROWS, N_TP, HQ * HD // N_TP).astype(jnp.float32)
    weight_groups = output_weight.reshape(N_TP, HQ * HD // N_TP, D).astype(jnp.float32)
    partial_value = jnp.einsum('btf,tfd->btd', attended_groups, weight_groups).astype(jnp.bfloat16)
    partial_value = lax.optimization_barrier(partial_value).astype(jnp.float32)
    mixed = lax.optimization_barrier(jnp.sum(partial_value, axis=1)).astype(jnp.bfloat16)
    return (mixed, new_key, new_value, new_gate)
```

```python
import functools

import jax
import jax.numpy as jnp
from jax import lax
from jax.experimental import pallas as pl
from jax.experimental.pallas import tpu as pltpu
from jax.sharding import PartitionSpec as P

EPSILON = 1e-06
FLOOR = -1e30
ROOT = 1
LANES = 128


f32, bf16 = jnp.float32, jnp.bfloat16


def params(mib=16):
    return pltpu.CompilerParams(vmem_limit_bytes=mib * 1024 * 1024)


def lane_index(shape):
    return lax.broadcasted_iota(jnp.int32, shape, len(shape) - 1)


def halves(x, half):
    low = lane_index(x.shape) < half
    a = jnp.sum(jnp.where(low, x, 0.0), axis=-1, keepdims=True)
    b = jnp.sum(jnp.where(low, 0.0, x), axis=-1, keepdims=True)
    return jnp.where(low, a, b), a, b


def split3(x):
    a = x.astype(bf16).astype(f32)
    b = (x - a).astype(bf16).astype(f32)
    c = (x - a - b).astype(bf16).astype(f32)
    return a, b, c


def project_kernel(seqs, place, tokens, gain, query_w, key_w, value_w, gate_w, out):
    tp = place[1]
    wide = tokens[...].astype(f32)
    scaled = (wide * gain[...].astype(f32)).astype(bf16)
    squares = jnp.sum(wide * wide, axis=1, keepdims=True)

    def dot(w):
        return jnp.dot(scaled, w, preferred_element_type=f32)

    chunks = query_w.shape[1] // LANES
    query = dot(query_w[...])
    for c in range(chunks):
        out[pl.ds(c, seqs, stride=chunks), :] = query[:, c * LANES : (c + 1) * LANES]
    base = seqs * chunks
    key, value, gate = dot(key_w[...]), dot(value_w[...]), dot(gate_w[...])
    half = LANES // 2
    tps = key.shape[1] // half
    key_here, value_here, gate_here = key[:, :half], value[:, :half], gate[:, :1]
    for t in range(1, tps):
        key_here = jnp.where(tp == t, key[:, t * half : (t + 1) * half], key_here)
        value_here = jnp.where(tp == t, value[:, t * half : (t + 1) * half], value_here)
        gate_here = jnp.where(tp == t, gate[:, t : t + 1], gate_here)
    out[base : base + 32, :] = jnp.zeros((32, LANES), f32)
    out[base : base + seqs, 0:half] = key_here
    out[base : base + seqs, half:LANES] = value_here
    lanes = lane_index((seqs, LANES))
    out[base + 16 : base + 16 + seqs, :] = jnp.where(lanes == 0, gate_here, jnp.where(lanes == 1, squares, 0.0))


def project(place, tokens, norm_gain, query_weight, key_weight, value_weight, gate_weight):
    seqs, width = tokens.shape
    rows = seqs * query_weight.shape[1] // LANES + 32
    whole = lambda x: pl.BlockSpec(x.shape, lambda i, s: (0,) * x.ndim)
    part = lambda x: pl.BlockSpec((width, x.shape[1]), lambda i, s: (s[0], 0))
    gain = norm_gain.reshape(1, width)
    return pl.pallas_call(
        functools.partial(project_kernel, seqs),
        grid_spec=pltpu.PrefetchScalarGridSpec(
            num_scalar_prefetch=1,
            grid=(1,),
            in_specs=[whole(tokens), whole(gain), whole(query_weight), part(key_weight), part(value_weight), part(gate_weight)],
            out_specs=pl.BlockSpec((rows, LANES), lambda i, s: (0, 0)),
        ),
        out_shape=jax.ShapeDtypeStruct((rows, LANES), f32),
        compiler_params=params(),
        name="project",
    )(place, tokens, gain, query_weight, key_weight, value_weight, gate_weight)


def finish_kernel(seqs, model, n, *refs):
    pieces, (query_gain, key_gain, out) = refs[:n], refs[n:]
    base = pieces[0].shape[0] - 32
    half = LANES // 2
    total = pieces[0][...]
    for p in pieces[1:]:
        total = total + p[...]
    query = total[:base]
    mean, _, _ = halves(query * query, half)
    factor = lax.rsqrt(mean * (1.0 / half) + EPSILON)
    out[0:base, :] = (query * factor * query_gain[...].astype(f32)).astype(bf16)
    kv = total[base : base + 16]
    extra = total[base + 16 : base + 32]
    mean, _, _ = halves(kv * kv, half)
    key = kv * lax.rsqrt(mean * (1.0 / half) + EPSILON) * key_gain[...].astype(f32)
    row_scale = lax.rsqrt(extra[:, 1:2] * (1.0 / model) + EPSILON)
    lanes = lane_index(kv.shape)
    out[base : base + 16, :] = jnp.where(lanes < half, key, kv * row_scale).astype(bf16)
    gate = row_scale * extra[:, 0:1]
    gate = jnp.minimum(gate, 0.0) - jnp.log1p(jnp.exp(-jnp.abs(gate)))
    a, b, c = split3(gate)
    out[base + 16 : base + 32, :] = jnp.where(
        lanes == 0, a, jnp.where(lanes == 1, b, jnp.where(lanes == 2, c, 0.0))
    ).astype(bf16)


def finish(pieces, seqs, model, query_gain, key_gain):
    twice = lambda g: jnp.concatenate([g, g]).reshape(1, LANES)
    return pl.pallas_call(
        functools.partial(finish_kernel, seqs, model, len(pieces)),
        out_shape=jax.ShapeDtypeStruct(pieces[0].shape, bf16),
        compiler_params=params(),
        name="finish",
    )(*pieces, twice(query_gain), twice(key_gain))


def attend_kernel(seqs, lengths, place, packed, decay, key_hbm, value_hbm, out, own_out, keys, values, scores, sems):
    half = LANES // 2
    chunks = 8
    base = seqs * chunks
    span = keys.shape[2]
    groups = [(0, seqs // 2), (seqs // 2, seqs)]
    copies = []
    for i, (src, dst) in enumerate(((key_hbm, keys), (value_hbm, values))):
        row = []
        for g, (lo, hi) in enumerate(groups):
            copy = pltpu.make_async_copy(src.at[pl.ds(lo, hi - lo), 0], dst.at[pl.ds(lo, hi - lo)], sems.at[i, g])
            copy.start()
            row.append(copy)
        copies.append(row)
    head_scale = float(half) ** (-0.5)
    gates = packed[base + 16 : base + 32, :].astype(f32)
    gates = gates[:, 0:1] + gates[:, 1:2] + gates[:, 2:3]
    kv = packed[base : base + 16, :].astype(f32)
    query = packed[0:base, :].astype(f32)
    lanes = lane_index((chunks, LANES))
    first = place[0] * span
    top_stat = jnp.zeros((chunks, LANES), f32)
    sum_stat = jnp.zeros((chunks, LANES), f32)
    own_stat = jnp.zeros((chunks, LANES), f32)
    for b in range(seqs):
        q = query[chunks * b : chunks * (b + 1)]
        k = kv[b : b + 1, 0:half]
        _, even, odd = halves(q * jnp.concatenate([k, k], axis=1), half)
        own_stat = jnp.where(lanes == 2 * b, even * head_scale, jnp.where(lanes == 2 * b + 1, odd * head_scale, own_stat))
    own_out[0:chunks, :] = own_stat
    own_out[chunks : chunks + 16, :] = kv
    positions = first + lax.broadcasted_iota(jnp.int32, (2 * chunks, span), 1)
    tops = {}
    for g, (lo, hi) in enumerate(groups):
        copies[0][g].wait()
        for b in range(lo, hi):
            q = query[chunks * b : chunks * (b + 1)]
            q = jnp.concatenate([q[:, :half], q[:, half:]], axis=0).astype(bf16)
            s = jnp.dot(q, keys[b], preferred_element_type=f32) * head_scale
            s = s + decay[b] + gates[b : b + 1, 0:1]
            s = jnp.where(positions < lengths[b], s, FLOOR)
            scores[b] = s
            top = jnp.max(s, axis=1, keepdims=True)
            tops[b] = top
            top_stat = jnp.where(lanes == 2 * b, top[:chunks], jnp.where(lanes == 2 * b + 1, top[chunks:], top_stat))
    for g, (lo, hi) in enumerate(groups):
        copies[1][g].wait()
        for b in range(lo, hi):
            w = jnp.where(positions < lengths[b], jnp.exp(scores[b] - tops[b]), 0.0)
            total = jnp.sum(w, axis=1, keepdims=True)
            sum_stat = jnp.where(lanes == 2 * b, total[:chunks], jnp.where(lanes == 2 * b + 1, total[chunks:], sum_stat))
            v = lax.dot_general(w.astype(bf16), values[b], (((1,), (1,)), ((), ())), preferred_element_type=f32)
            out[chunks * b : chunks * (b + 1), :] = jnp.concatenate([v[:chunks], v[chunks:]], axis=1).astype(bf16)
    write_stats(out, base, seqs, top_stat, sum_stat)


def write_stats(out, base, seqs, top, total):
    lanes = lane_index(top.shape)
    step = 2 * seqs
    pieces = [*split3(top), *split3(total)[:2]]
    packed = jnp.zeros(top.shape, f32)
    for i, p in enumerate(pieces):
        moved = pltpu.roll(p, i * step, 1) if i else p
        packed = jnp.where((lanes >= i * step) & (lanes < (i + 1) * step), moved, packed)
    out[base : base + 16, :] = jnp.concatenate([packed, jnp.zeros(packed.shape, f32)], axis=0).astype(bf16)


def read_stats(ref, base, seqs):
    packed = ref[base : base + 16, :].astype(f32)[:8]
    step = 2 * seqs
    p = [packed] + [pltpu.roll(packed, LANES - i * step, 1) for i in range(1, 5)]
    return p[0] + p[1] + p[2], p[3] + p[4]


def attend(place, lengths, packed, decay_cache, key_cache, value_cache):
    seqs = key_cache.shape[0]
    span = key_cache.shape[3]
    dim = key_cache.shape[2]
    rows = packed.shape[0] - 16
    smem = pl.BlockSpec(memory_space=pltpu.SMEM)
    vmem = pl.BlockSpec(memory_space=pltpu.VMEM)
    hbm = pl.BlockSpec(memory_space=pl.ANY)
    return pl.pallas_call(
        functools.partial(attend_kernel, seqs),
        in_specs=[smem, smem, vmem, vmem, hbm, hbm],
        out_specs=[vmem, vmem],
        out_shape=[jax.ShapeDtypeStruct((rows, LANES), bf16), jax.ShapeDtypeStruct((24, LANES), f32)],
        scratch_shapes=[
            pltpu.VMEM((seqs, dim, span), bf16),
            pltpu.VMEM((seqs, dim, span), bf16),
            pltpu.VMEM((seqs, 16, span), f32),
            pltpu.SemaphoreType.DMA((2, 2)),
        ],
        compiler_params=params(),
        name="attend",
    )(lengths, place, packed, decay_cache, key_cache, value_cache)


def merge_kernel(seqs, n, last, *refs):
    pieces, refs = refs[:n], refs[n:]
    half = LANES // 2
    base = pieces[0].shape[0] - 16
    stats = [read_stats(p, base, seqs) for p in pieces]
    top = stats[0][0]
    for m, _ in stats[1:]:
        top = jnp.maximum(top, m)
    if last:
        own, out = refs
        own_stat = own[0:8, :]
        top = jnp.maximum(top, own_stat)
        own_scale = jnp.exp(own_stat - top)
    else:
        (out,) = refs
    scales = [jnp.exp(m - top) for m, _ in stats]
    total = stats[0][1] * scales[0]
    for (_, t), s in zip(stats[1:], scales[1:]):
        total = total + t * s
    if last:
        total = total + own_scale
        inverse = 1.0 / total
        kv = own[8:24, :]
    low = lane_index((8, LANES)) < half

    def wide(x, b):
        return jnp.where(low, x[:, 2 * b : 2 * b + 1], x[:, 2 * b + 1 : 2 * b + 2])

    for b in range(seqs):
        summed = None
        for p, s in zip(pieces, scales):
            v = p[8 * b : 8 * (b + 1), :].astype(f32) * wide(s, b)
            summed = v if summed is None else summed + v
        if last:
            v = kv[b : b + 1, half:LANES]
            summed = summed + wide(own_scale, b) * jnp.concatenate([v, v], axis=1)
            summed = summed * wide(inverse, b)
        out[8 * b : 8 * (b + 1), :] = summed.astype(bf16)
    if not last:
        write_stats(out, base, seqs, top, total)


def merge(pieces, seqs, own=None):
    last = own is not None
    rows = pieces[0].shape[0] - (16 if last else 0)
    return pl.pallas_call(
        functools.partial(merge_kernel, seqs, len(pieces), last),
        out_shape=jax.ShapeDtypeStruct((rows, LANES), bf16),
        compiler_params=params(),
        name="merge_last" if last else "merge",
    )(*pieces, *([own] if last else []))


def output_kernel(seqs, n, *refs):
    pieces, (weight, out, scratch) = refs[:n], refs[n:]
    total = pieces[0][...].astype(f32)
    for p in pieces[1:]:
        total = total + p[...].astype(f32)
    scratch[...] = total
    acc = jnp.zeros((seqs, weight.shape[1]), f32)
    for c in range(8):
        left = scratch[pl.ds(c, seqs, stride=8), :].astype(bf16)
        acc = acc + jnp.dot(left, weight[c * LANES : (c + 1) * LANES, :], preferred_element_type=f32)
    out[...] = acc.astype(bf16)


def project_out(pieces, weight, seqs):
    return pl.pallas_call(
        functools.partial(output_kernel, seqs, len(pieces)),
        out_shape=jax.ShapeDtypeStruct((seqs, weight.shape[1]), bf16),
        scratch_shapes=[pltpu.VMEM(pieces[0].shape, f32)],
        compiler_params=params(),
        name="project_out",
    )(*pieces, weight)


def plan(count):
    leaders = list(range(3, count - 3, 3))
    alone = list(range(leaders[-1] + 2, count - 1))
    far = lambda u: -min(u, count - u)
    return sorted(leaders, key=far), sorted(alone, key=far)


def move(array, axis, pairs):
    count = lax.axis_size(axis)
    return lax.ppermute(array, axis, [((s + ROOT) % count, (d + ROOT) % count) for s, d in pairs])


def spread(array, axis):
    count = lax.axis_size(axis)
    leaders, alone = plan(count)
    is_root = lax.axis_index(axis) == ROOT
    pieces = [move(array, axis, [(0, u)]) for u in leaders + alone]
    got = pieces[0]
    for piece in pieces[1:]:
        got = got + piece
    got = jnp.where(is_root, array, got)
    up = move(got, axis, [(u, u + 1) for u in [0] + leaders])
    down = move(got, axis, [(u, (u - 1) % count) for u in [0] + leaders])
    return [got, up, down]


def on_device(
    tokens, norm_gain, query_weight, key_weight, value_weight, gate_weight, output_weight,
    query_gain, key_gain, key_cache, value_cache, decay_cache, lengths,
):
    head_dim = query_gain.shape[0]
    seqs, width_here = tokens.shape
    kv_here = key_cache.shape[1]
    n = lax.axis_size("kv")
    model = width_here * n
    place = jnp.stack([lax.axis_index("kv"), lax.axis_index("tp")]).astype(jnp.int32)
    part = project(place, tokens, norm_gain, query_weight, key_weight, value_weight, gate_weight)

    direct = [move(part, "kv", [(u, 0)]) for u in (n - 2, n - 3, n - 1)]
    led = list(range(3, n - 3, 3))
    g1 = move(part, "kv", [(u + 1, u) for u in led if u + 1 < n - 3] + [(1, 0)])
    g2 = move(part, "kv", [(u - 1, u) for u in led])
    joint = part + g1 + g2
    firsts = [move(joint, "kv", [(u, 0)]) for u in reversed(led)]
    packed = finish([joint] + firsts + direct[::-1], seqs, model, query_gain, key_gain)
    a, b, c = spread(packed, "kv")
    packed = a + b + c

    base = packed.shape[0] - 32
    new_key = packed[base : base + seqs, :head_dim].reshape(seqs, kv_here, head_dim)
    new_value = packed[base : base + seqs, head_dim:].reshape(seqs, kv_here, head_dim)
    gates = packed[base + 16 : base + 16 + seqs, :3].astype(f32)
    new_gate = gates[:, 0:1] + gates[:, 1:2] + gates[:, 2:3]

    sent, own = attend(place, lengths, packed, decay_cache, key_cache, value_cache)
    leaders, alone = plan(n)
    up = move(sent, "kv", [((k - 1) % n, k) for k in [0] + leaders])
    down = move(sent, "kv", [(k + 1, k) for k in [0] + leaders])
    lone = [move(sent, "kv", [(k, 0)]) for k in alone]
    joint = merge([sent, up, down], seqs)
    firsts = [move(joint, "kv", [(k, 0)]) for k in leaders]
    attended = merge([joint] + firsts + lone, seqs, own)
    partial_value = project_out(spread(attended, "kv"), output_weight, seqs)
    n_tp = lax.axis_size("tp")
    mixed = partial_value.astype(f32)
    for d in range(1, n_tp):
        mixed = mixed + lax.ppermute(partial_value, "tp", [(i, (i + d) % n_tp) for i in range(n_tp)]).astype(f32)
    return (mixed.astype(bf16), new_key, new_value, new_gate)


def solution(mesh):
    in_specs = (
        P(("grp", "dp"), "kv"), P("kv"), P("kv", "tp"), P(), P(), P(), P("tp", "kv"), P(), P(),
        P(("grp", "dp"), "tp", None, "kv"), P(("grp", "dp"), "tp", None, "kv"), P(("grp", "dp"), "tp", "kv"),
        P(("grp", "dp")),
    )
    out_specs = (
        P(("grp", "dp"), "kv"), P(("grp", "dp"), "tp", None), P(("grp", "dp"), "tp", None), P(("grp", "dp"), "tp"),
    )
    return jax.shard_map(on_device, mesh=mesh, in_specs=in_specs, out_specs=out_specs, check_vma=False)
```
